32 devices in a mesh: gr: 2 (over y), fs: 8 (over z, core), tp: 2 (over x).
Axes of the slice: x: 2, y: 2, z: 4, core: 2. Of those that a mesh axis runs over, the one named last changes fastest.
Arguments:
- prompt: bfloat16 [2048, 2048], P(('gr', 'fs')), may hold values from -6 to 6
- expert_ids: int32 [2048, 2], P(('gr', 'fs')), may hold values from 0 to 7, all different within a row; in each aligned block of 128 rows (0 to 127, 128 to 255, ...) at most 32 rows name the same one
- route_weights: float32 [2048, 2], P(('gr', 'fs')), may hold values from 0.2 to 1
- gate_master: float32 [8, 2048, 8192], P('gr', 'fs', 'tp'), may hold values from -0.125 to 0.125
- up_master: float32 [8, 2048, 8192], P('gr', 'fs', 'tp'), may hold values from -0.125 to 0.125
- down_master: float32 [8, 8192, 2048], P('gr', 'fs', 'tp'), may hold values from -0.0625 to 0.0625
- ffn_gain: float32 [2048], P('fs'), may hold values from 0.1 to 1.9
Outputs:
- gate_serving: bfloat16 [8, 2048, 8192], P('tp', None, 'fs')
- up_serving: bfloat16 [8, 2048, 8192], P('tp', None, 'fs')
- down_serving: bfloat16 [8, 8192, 2048], P('tp', 'fs')
- mixed: bfloat16 [2048, 2048], P(('gr', 'fs', 'tp'))
The draws below stay inside these ranges and needn't reach their ends.
Inputs may be any that keep to these rules, and one draw needn't show every extreme that they name: `expert_ids`: the two experts of a token differ; the rows of one index of gr and fs name each expert exactly 32 times.
All inputs are finite; a program needn't handle non-finite values.
Results may differ from the reference program's by a relative error of at most 0.025.
Values may be sent and summed in bfloat16 or wider, within the bound.
No kernel may reach another device: no remote copies, remote signals or barrier semaphores. Data moves between devices by JAX's collectives and lax.ppermute only.
A program may use at most 256 MiB of HBM per device.

```python
import math
import jax
import jax.numpy as jnp
import numpy as np
from jax import lax

D = 2048
FF = 8192
EXPERTS = 8
TOK_DEV = 128
SLOTS = 32
TOKENS = 2048
N_FS = 8


def block_scale(own_key, dims, cuts, low, largest):
    gain, own = 1.0, jax.random.fold_in(own_key, 6)
    for axis_at, parts in cuts:
        steps = jnp.exp(jax.random.uniform(jax.random.fold_in(own, axis_at), (parts,), jnp.float32, low / len(cuts), largest / len(cuts)))
        gain = gain * jnp.repeat(steps, dims[axis_at] // parts).reshape([-1 if axis == axis_at else 1 for axis in range(len(dims))])
    return gain


def deal_out(stream_key, own, number, rows, amount, top, reach, slope):
    sequence = jax.random.permutation(stream_key, amount)
    heavy_load, ordinary = load_shares(amount, rows * top, reach, slope, True), load_shares(amount, rows * top, reach, slope, False)
    places = jnp.arange(amount)

    def named(tallies, offset_by):
        used = int((tallies > 0).sum())
        fixed = max(1, used // 4)
        shifted = fixed + (places - fixed + offset_by * (used - fixed)) % max(1, amount - fixed)
        return jnp.zeros((amount,), jnp.int32).at[sequence[jnp.where(places < fixed, places, shifted)]].set(jnp.asarray(tallies, jnp.int32))

    tallies = jnp.where(number % 4 == 0, named(heavy_load, number // 4), named(ordinary, number - number // 4 - 1))
    mixed = jax.random.permutation(jax.random.fold_in(own, 3), amount)
    giver, sink = mixed[0:amount // 2 * 2:2], mixed[1:amount // 2 * 2:2]
    margin = jnp.minimum(tallies[giver] - 1, reach - tallies[sink]) // 2
    margin = jnp.where((giver == sequence[0]) | (sink == sequence[0]) | (tallies[sink] == 0), 0, jnp.maximum(margin, 0))
    shifted = jax.random.randint(jax.random.fold_in(own, 4), (amount // 2,), 0, 1 << 20) % (margin + 1)
    tallies = tallies.at[giver].add(-shifted).at[sink].add(shifted)
    items = jnp.searchsorted(jnp.cumsum(tallies), jnp.arange(rows * top), side="right").astype(jnp.int32)
    grid = items.reshape(top, rows).T
    grid = grid[jax.random.permutation(jax.random.fold_in(own, 1), rows)]
    offset_by = jax.random.randint(jax.random.fold_in(own, 2), (rows, 1), 0, top)
    return jnp.take_along_axis(grid, (jnp.arange(top)[None, :] + offset_by) % top, axis=1)


def load_shares(amount, total, bound, skew, full):
    portions = [(1 << 20) // math.isqrt(grade ** skew) + 1 for grade in range(1, amount + 1)]
    largest = bound if full else min(bound, max(-(-total // amount), total * portions[0] // sum(portions)))
    least = 1 if total - largest >= amount - 1 else 0
    holding, spare = [largest] + [least] * (amount - 1), total - largest - least * (amount - 1)
    while spare > 0:
        free = [i for i in range(1, amount) if holding[i] < largest] or [i for i in range(1, amount) if holding[i] < bound]
        whole, left = sum([portions[i] for i in free]), spare
        for i in free:
            more = min(bound - holding[i], max(1, left * portions[i] // whole), spare)
            holding[i] = holding[i] + more
            spare = spare - more
    return np.array(holding)


def gaussian(stream_key, extent, scale, limit, pieces=(), kind=jnp.bfloat16):
    factor_of = block_scale(stream_key, extent, pieces, -0.22, 0.18) if pieces else 1.0
    drawn = jax.random.normal(stream_key, extent, jnp.float32) * scale * factor_of
    return jnp.minimum(jnp.maximum(drawn, -limit), limit).astype(kind)


def setup_inputs(seed: int = 0) -> dict:
    keys = jax.random.split(jax.random.key(seed), 8)
    prompt = gaussian(keys[0], (TOKENS, D), 1.0, 6.0, ((0, 16),))
    expert_ids_keys = jax.random.split(jax.random.fold_in(keys[1], 1), TOKENS // TOK_DEV)
    expert_ids_turns = jax.random.permutation(jax.random.fold_in(keys[1], 3), TOKENS // TOK_DEV)
    expert_ids = jax.vmap(lambda own, number: deal_out(jax.random.fold_in(keys[1], 2), own, number, TOK_DEV, EXPERTS, 2, SLOTS, 0))(expert_ids_keys, expert_ids_turns).reshape((TOKENS, 2))
    route_weights = jnp.clip(0.2 + 0.8 * jax.random.uniform(keys[2], (TOKENS, 2), jnp.float32) ** block_scale(keys[2], (TOKENS, 2), ((0, 16),), -0.2, 0.2), 0.2, 1.0)
    gate_master = gaussian(keys[3], (EXPERTS, D, FF), D ** -0.5, 0.125, ((0, 2), (1, 8), (2, 2)), jnp.float32)
    up_master = gaussian(keys[4], (EXPERTS, D, FF), D ** -0.5, 0.125, ((0, 2), (1, 8), (2, 2)), jnp.float32)
    down_master = gaussian(keys[5], (EXPERTS, FF, D), FF ** -0.5, 0.0625, ((0, 2), (1, 8), (2, 2)), jnp.float32)
    ffn_gain = jnp.clip(1.0 + 0.18 * jax.random.normal(keys[6], (D,), jnp.float32), 0.1, 1.9)
    return dict(prompt=prompt, expert_ids=expert_ids, route_weights=route_weights, gate_master=gate_master, up_master=up_master, down_master=down_master, ffn_gain=ffn_gain)


NORM_EPS = 1e-06

def reference(prompt, expert_ids, route_weights, gate_master, up_master, down_master, ffn_gain):
    folding = ffn_gain[None, :, None]
    gate_serving = (gate_master * folding).astype(jnp.bfloat16)
    up_serving = (up_master * folding).astype(jnp.bfloat16)
    down_serving = down_master.astype(jnp.bfloat16)
    xfloat = prompt.astype(jnp.float32)
    normed = (xfloat * lax.rsqrt(lax.optimization_barrier(jnp.mean(xfloat * xfloat, axis=1, keepdims=True)) + NORM_EPS)).astype(jnp.bfloat16)
    pair_expert = expert_ids.reshape(-1)
    pair_weight = route_weights.reshape(-1)
    chosen = TOKENS * 2 // EXPERTS
    slice_width = FF // N_FS
    terms = jnp.zeros((TOKENS * 2, D), jnp.bfloat16)
    for expert in range(EXPERTS):
        ordering = jnp.argsort((pair_expert != expert).astype(jnp.int32), stable=True)[:chosen].astype(jnp.int32)
        rows_in = normed[ordering // 2]
        gate_part = jnp.dot(rows_in, gate_serving[expert], preferred_element_type=jnp.float32)
        up_part = jnp.dot(rows_in, up_serving[expert], preferred_element_type=jnp.float32)
        hidden = (jax.nn.silu(gate_part) * up_part).astype(jnp.bfloat16)
        down_one = down_serving[expert]

        def add_slice(total, index):
            start_row = (index * slice_width).astype(jnp.int32)
            hidden_block = lax.dynamic_slice_in_dim(hidden, start_row, slice_width, 1)
            weights = lax.dynamic_slice_in_dim(down_one, start_row, slice_width, 0)
            partial_sum = lax.optimization_barrier(jnp.dot(hidden_block, weights, preferred_element_type=jnp.float32).astype(jnp.bfloat16))
            return (total + partial_sum.astype(jnp.float32), None)
        expert_out, _ = lax.scan(add_slice, jnp.zeros((chosen, D), jnp.float32), jnp.arange(N_FS, dtype=jnp.int32))
        terms = terms.at[ordering].set((expert_out * pair_weight[ordering][:, None]).astype(jnp.bfloat16))
    mixed = lax.optimization_barrier(jnp.sum(terms.reshape(TOKENS, 2, D).astype(jnp.float32), axis=1)).astype(jnp.bfloat16)
    return (gate_serving, up_serving, down_serving, mixed)
```

```python
import functools

import jax
import jax.numpy as jnp
from jax import lax
from jax.experimental import pallas as pl
from jax.experimental.pallas import tpu as pltpu
from jax.sharding import PartitionSpec as P


NORM_EPS = 1e-06
SLOTS = 32
CUT_EIGHTHS = 4


ANY = pl.BlockSpec(memory_space=pl.ANY)
SMEM = pl.BlockSpec(memory_space=pltpu.SMEM)
VMEM = pl.BlockSpec(memory_space=pltpu.VMEM)
BF16 = jnp.bfloat16
F32 = jnp.float32


def rotate(value, axis, step):
    count = lax.axis_size(axis)
    return lax.ppermute(value, axis, [(i, (i + step) % count) for i in range(count)])


def pack_kernel(parts, where_ref, after_ref, *refs):
    masters, gains, outs = refs[:parts], refs[parts : 2 * parts], refs[2 * parts :]
    for master, gain, out in zip(masters, gains, outs):
        out[0, 0] = (master[0] * gain[...]).astype(BF16)


def pack(master, gain, where, unit, units, width, parts, after):
    _, rows, cols = master.shape
    held, blocks, part_rows = master.shape[0] // units, cols // width, rows // parts

    def row_part(p):
        return lambda k, c, w: (k * units + unit, (w[0] + p) % parts, c)

    def gain_part(p):
        return lambda k, c, w: ((w[0] + p) % parts, 0)

    out_spec = pl.BlockSpec((1, 1, part_rows, width), lambda k, c, w: (k, c, 0, 0))
    return pl.pallas_call(
        functools.partial(pack_kernel, parts),
        grid_spec=pltpu.PrefetchScalarGridSpec(
            num_scalar_prefetch=1,
            grid=(held, blocks),
            in_specs=[ANY]
            + [pl.BlockSpec((1, part_rows, width), row_part(p)) for p in range(parts)]
            + [pl.BlockSpec((part_rows, 1), gain_part(p)) for p in range(parts)],
            out_specs=[out_spec] * parts,
        ),
        out_shape=[jax.ShapeDtypeStruct((held, blocks, part_rows, width), BF16)] * parts,
        name="pack",
    )(where, after, *([master] * parts), *([gain] * parts))


def choose_kernel(group_count, tp_count, held, tp_step, where_ref, after_ref, *refs):
    by_gr, (out, stage, sem) = refs[:group_count], refs[group_count:]
    target = lax.rem(where_ref[2] + tp_step, tp_count)
    gr_step = lax.rem(where_ref[0] + group_count - lax.div(target, held), group_count)
    for s in range(group_count):

        @pl.when(gr_step == s)
        def _(s=s):
            copy = pltpu.make_async_copy(by_gr[s].at[lax.rem(target, held)], stage, sem)
            copy.start()
            copy.wait()

    copy = pltpu.make_async_copy(stage, out, sem)
    copy.start()
    copy.wait()


def choose(by_gr, where, tp_step, after):
    held, *shape = by_gr[0].shape
    return pl.pallas_call(
        functools.partial(choose_kernel, len(by_gr), lax.axis_size("tp"), held, tp_step),
        in_specs=[SMEM] + [ANY] * (len(by_gr) + 1),
        out_specs=ANY,
        out_shape=jax.ShapeDtypeStruct(tuple(shape), BF16),
        scratch_shapes=[pltpu.VMEM(tuple(shape), BF16), pltpu.SemaphoreType.DMA],
        name="choose",
    )(where, after, *by_gr)


def stack_kernel(count, after_ref, *refs):
    ins, (out, stage, in_sem, out_sem) = refs[:count], refs[count:]

    def fetch(i):
        return pltpu.make_async_copy(ins[i], stage.at[i], in_sem.at[i])

    def flush(i):
        return pltpu.make_async_copy(stage.at[i], out.at[i], out_sem.at[i])

    for i in range(count):
        fetch(i).start()
    for i in range(count):
        fetch(i).wait()
        flush(i).start()
    for i in range(count):
        flush(i).wait()


def stack(values, after):
    count, shape = len(values), (len(values), *values[0].shape)
    return pl.pallas_call(
        functools.partial(stack_kernel, count),
        in_specs=[ANY] * (count + 1),
        out_specs=ANY,
        out_shape=jax.ShapeDtypeStruct(shape, BF16),
        scratch_shapes=[
            pltpu.VMEM(shape, BF16),
            pltpu.SemaphoreType.DMA((count,)),
            pltpu.SemaphoreType.DMA((count,)),
        ],
        name="stack",
    )(after, *values)


def split_kernel(group_count, tp_count, shard_count, held, where_ref, after_ref, *refs):
    by_gr, by_tp = refs[:group_count], refs[group_count : group_count + tp_count - 1]
    outs = refs[group_count + tp_count - 1 : group_count + tp_count - 1 + shard_count]
    stage, in_sem, out_sem = refs[-3:]
    g, f, t = where_ref[0], where_ref[1], where_ref[2]
    blocks = by_gr[0].shape[1]

    def source(step):
        target = lax.rem(f + step, shard_count)
        return lax.div(target, blocks), lax.rem(target, blocks)

    for step in range(shard_count):
        column, block = source(step)
        own_gr = lax.rem(g + group_count - lax.div(t, held), group_count)
        tp_step = lax.rem(t + tp_count - column, tp_count)
        for s in range(group_count):

            @pl.when((tp_step == 0) & (own_gr == s))
            def _(s=s):
                pltpu.make_async_copy(
                    by_gr[s].at[lax.rem(t, held), block], stage.at[step], in_sem.at[step]
                ).start()

        for s in range(1, tp_count):

            @pl.when(tp_step == s)
            def _(s=s):
                pltpu.make_async_copy(by_tp[s - 1].at[block], stage.at[step], in_sem.at[step]).start()

    for step in range(shard_count):
        pltpu.make_async_copy(stage.at[step], stage.at[step], in_sem.at[step]).wait()
        pltpu.make_async_copy(stage.at[step], outs[step], out_sem.at[step]).start()
    for step in range(shard_count):
        pltpu.make_async_copy(stage.at[step], outs[step], out_sem.at[step]).wait()


def split(by_gr, by_tp, where, shard_count, after):
    held, _, rows, width = by_gr[0].shape
    piece = jax.ShapeDtypeStruct((rows, width), BF16)
    return pl.pallas_call(
        functools.partial(split_kernel, len(by_gr), len(by_tp) + 1, shard_count, held),
        in_specs=[SMEM] + [ANY] * (len(by_gr) + len(by_tp) + 1),
        out_specs=[ANY] * shard_count,
        out_shape=[piece] * shard_count,
        scratch_shapes=[
            pltpu.VMEM((shard_count, rows, width), BF16),
            pltpu.SemaphoreType.DMA((shard_count,)),
            pltpu.SemaphoreType.DMA((shard_count,)),
        ],
        name="split",
    )(where, after, *by_gr, *by_tp)


def up_kernel(counts, shard_count, parts, unit, fresh, where_ref, after_ref, near, far, *refs):
    gate_in, up_in = refs[: counts[0]], refs[counts[0] : sum(counts)]
    rest = refs[sum(counts) :]
    if not fresh:
        rest = rest[2:]
    gate_out, up_out, hidden_ref, tokens, gate_buf, up_buf, token_sem, in_sem, out_sem = rest
    g, f = where_ref[0], where_ref[1]
    whole = gate_buf.shape[0] // shard_count
    sides = ((gate_in, gate_buf, gate_out), (up_in, up_buf, up_out))

    def place(index, side):
        part, step = divmod(index, shard_count)
        rows = whole // parts[side]
        source = lax.rem(f + shard_count - step, shard_count)
        start = source * whole + lax.rem(g + parts[side] - part, parts[side]) * rows
        return pl.ds(pl.multiple_of(start, rows), rows)

    def fetch(index, side):
        ins, buf, _ = sides[side]
        part, step = divmod(index, shard_count)
        src = ins[index] if parts[side] == 1 else ins[part].at[step]
        return pltpu.make_async_copy(src, buf.at[place(index, side)], in_sem.at[side, index])

    def flush(index, side):
        _, buf, out = sides[side]
        at = place(index, side)
        return pltpu.make_async_copy(buf.at[at], out.at[unit, at, :], out_sem.at[side, index])

    outer, slots, depth = near.shape[0], tokens.shape[1], tokens.shape[2]
    rows_of_unit = pl.ds(unit * slots, slots)
    token_copies = [
        pltpu.make_async_copy(
            src.at[:, rows_of_unit, :], tokens.at[pl.ds(i * outer, outer)], token_sem.at[i]
        )
        for i, src in enumerate((near, far))
    ]
    for copy in token_copies:
        copy.start()
    for side in (0, 1):
        for index in range(shard_count * parts[side]):
            fetch(index, side).start()
    for copy in token_copies:
        copy.wait()
    rows_in = tokens[...].reshape(2 * outer * slots, depth)
    products = []
    for side in (0, 1):
        for index in range(shard_count * parts[side]):
            fetch(index, side).wait()
            flush(index, side).start()
        products.append(jnp.dot(rows_in, sides[side][1][...], preferred_element_type=F32))
    gate, up = products
    hidden_ref[...] = (gate / (1.0 + jnp.exp(-gate)) * up).astype(BF16)
    for side in (0, 1):
        for index in range(shard_count * parts[side]):
            flush(index, side).wait()


def up_project(where, near, far, gate_pieces, up_pieces, outs, unit, parts, out_shape, after):
    width = out_shape.shape[2]
    shard_count, depth = 2 * near.shape[0], near.shape[2]
    slots = near.shape[1] // out_shape.shape[0]
    token_count = shard_count * slots
    counts = (len(gate_pieces), len(up_pieces))
    fresh = outs is None
    operands = [where, after, near, far, *gate_pieces, *up_pieces] + ([] if fresh else list(outs))
    return pl.pallas_call(
        functools.partial(up_kernel, counts, shard_count, parts, unit, fresh),
        in_specs=[SMEM] + [ANY] * (len(operands) - 1),
        out_specs=[ANY, ANY, VMEM],
        out_shape=[out_shape, out_shape, jax.ShapeDtypeStruct((token_count, width), BF16)],
        scratch_shapes=[
            pltpu.VMEM((shard_count, slots, depth), BF16),
            pltpu.VMEM((depth, width), BF16),
            pltpu.VMEM((depth, width), BF16),
            pltpu.SemaphoreType.DMA((2,)),
            pltpu.SemaphoreType.DMA((2, shard_count * max(parts))),
            pltpu.SemaphoreType.DMA((2, shard_count * max(parts))),
        ],
        input_output_aliases={} if fresh else {4 + sum(counts): 0, 5 + sum(counts): 1},
        name="up_project",
    )(*operands)


def down_kernel(group_count, tp_count, held, unit, fresh, where_ref, after_ref, hidden_ref, *refs):
    by_gr, by_tp = refs[:group_count], refs[group_count : group_count + tp_count - 1]
    rest = refs[group_count + tp_count - 1 :]
    if not fresh:
        rest = rest[1:]
    down_out, near_ref, far_ref, buf, part, in_sem, out_sem = rest
    g, t = where_ref[0], where_ref[2]
    cols = buf.shape[2]
    own_gr = lax.rem(g + group_count - lax.div(t, held), group_count)
    for s in range(group_count):

        @pl.when(own_gr == s)
        def _(s=s):
            pltpu.make_async_copy(by_gr[s].at[lax.rem(t, held)], buf.at[0], in_sem.at[0]).start()

    for s in range(1, tp_count):
        pltpu.make_async_copy(by_tp[s - 1], buf.at[s], in_sem.at[s]).start()

    def flush(s):
        column = pl.multiple_of(lax.rem(t + tp_count - s, tp_count) * cols, cols)
        return pltpu.make_async_copy(
            buf.at[s], down_out.at[unit, :, pl.ds(column, cols)], out_sem.at[s]
        )

    for s in range(tp_count):
        pltpu.make_async_copy(buf.at[s], buf.at[s], in_sem.at[s]).wait()
        flush(s).start()
        column = pl.multiple_of(lax.rem(t + tp_count - s, tp_count) * cols, cols)
        part[:, pl.ds(column, cols)] = jnp.dot(
            hidden_ref[...], buf[s], preferred_element_type=F32
        ).astype(BF16)
    half = near_ref.shape[0]
    near_ref[...] = part[:half]
    far_ref[...] = part[half:]
    for s in range(tp_count):
        flush(s).wait()


def down_project(where, hidden, by_gr, by_tp, out, unit, out_shape, after):
    held, rows, cols = by_gr[0].shape
    token_count, _ = hidden.shape
    tp_count = len(by_tp) + 1
    depth = cols * tp_count
    fresh = out is None
    half = jax.ShapeDtypeStruct((token_count // 2, depth), BF16)
    operands = [where, after, hidden, *by_gr, *by_tp] + ([] if fresh else [out])
    return pl.pallas_call(
        functools.partial(down_kernel, len(by_gr), tp_count, held, unit, fresh),
        in_specs=[SMEM, ANY, VMEM] + [ANY] * (len(operands) - 3),
        out_specs=[ANY, VMEM, VMEM],
        out_shape=[out_shape, half, half],
        scratch_shapes=[
            pltpu.VMEM((tp_count, rows, cols), BF16),
            pltpu.VMEM((token_count, depth), BF16),
            pltpu.SemaphoreType.DMA((tp_count,)),
            pltpu.SemaphoreType.DMA((tp_count,)),
        ],
        input_output_aliases={} if fresh else {len(operands) - 1: 0},
        name="down_project",
    )(*operands)


def fold_kernel(outer, after_ref, keep_ref, other_ref, own_ref, *sends):
    total = keep_ref[...].astype(F32) + other_ref[...].astype(F32)
    slots = own_ref.shape[0]
    own_ref[...] = total[:slots]
    for step in range(1, outer):
        sends[step - 1][...] = total[step * slots : (step + 1) * slots].astype(BF16)


def fold(keep, other, outer, after):
    slots, depth = keep.shape[0] // outer, keep.shape[1]
    return pl.pallas_call(
        functools.partial(fold_kernel, outer),
        in_specs=[ANY, VMEM, VMEM],
        out_specs=[VMEM] * outer,
        out_shape=[jax.ShapeDtypeStruct((slots, depth), F32)]
        + [jax.ShapeDtypeStruct((slots, depth), BF16)] * (outer - 1),
        name="fold",
    )(after, keep, other)


def combine_kernel(count, first, after_ref, weight_ref, onehot_ref, own_ref, *refs):
    others, (mixed_ref, out_ref) = refs[:count], refs[-2:]
    total = own_ref[...]
    for other in others:
        total = total + other[...].astype(F32)
    term = (total * weight_ref[...]).astype(BF16)
    share = lax.dot_general(
        onehot_ref[...], term, (((1,), (0,)), ((), ())), preferred_element_type=F32
    )
    out_ref[...] = share if first else mixed_ref[...] + share


def combine(weight, onehot, own, others, mixed, after):
    shape = jax.ShapeDtypeStruct((onehot.shape[0], own.shape[1]), F32)
    first = mixed is None
    operands = [after, weight, onehot, own, *others, own if first else mixed]
    return pl.pallas_call(
        functools.partial(combine_kernel, len(others), first),
        in_specs=[ANY] + [VMEM] * (len(operands) - 1),
        out_specs=VMEM,
        out_shape=shape,
        name="combine",
    )(*operands)


def cast_kernel(after_ref, in_ref, out_ref):
    out_ref[...] = in_ref[...].astype(BF16)


def cast(master, unit, units, after):
    local_in, rows, cols = master.shape
    held, half = local_in // units, rows // 2
    return pl.pallas_call(
        cast_kernel,
        grid=(held, 2),
        in_specs=[ANY, pl.BlockSpec((1, half, cols), lambda k, i: (k * units + unit, i, 0))],
        out_specs=pl.BlockSpec((1, half, cols), lambda k, i: (k, i, 0)),
        out_shape=jax.ShapeDtypeStruct((held, rows, cols), BF16),
        name="cast",
    )(after, master)


def plan(units, cut):
    both = (0, 1)
    keys = [(which, unit) for unit in range(units) for which in both]
    first = [key for key in keys if key in cut]
    second = [key for key in keys if key not in cut]
    cut_rank = {unit: sum((which, unit) in cut for which in both) for unit in range(units)}
    downs = sorted(range(units), key=lambda unit: (cut_rank[unit], unit))
    events = []
    y = x = z = 0.3
    ready = {}
    for i, key in enumerate(first):
        events.append((0.2 * i, "pack", key))
        y = max(y, 0.2 * i + 0.3) + 1
        ready["y", key] = y
    start = 0.2 * min(2, len(first))
    events.append((start + 0.01, "tokens", None))
    z = start + 2.3
    events.append((z, "near", None))
    for i, key in enumerate(second):
        at = max(0.2 * len(first), 0.9) + 0.3 * i
        events.append((at, "pack", key))
        y = max(y, at + 0.3) + 2
        ready["y", key] = y
    for i, unit in enumerate(downs):
        events.append((max(0.2 * len(first), 0.9) + 0.3 * (len(second) + i) + 0.2, "cast", unit))
        y = y + 2
        ready["y", unit] = y
    for key in first + second + downs:
        size = 1 if key in first else 2
        at = ready["y", key]
        events.append((at, "choose", key))
        x = max(x, at + 0.2) + size
        ready["x", key] = x
        if key not in downs:
            events.append((x, "split", key))
            z = max(z, x + 0.2) + 2 * size
            ready["z", key] = z
    for key in first:
        at = ready["z", key]
        events.append((at, "stack", key))
        y = max(y, at + 0.2) + 2
        ready["z", key] = y
    order = sorted(range(units), key=lambda unit: max(ready["z", (which, unit)] for which in both))
    now = 0.0
    for unit in order:
        at = max(now, ready["x", unit], *(ready["z", (which, unit)] for which in both))
        now = at + 0.7
        events.append((at, "project", unit))
        z = max(z, at + 0.7) + 0.5
        events.append((z + 0.3, "settle", unit))
    events.sort(key=lambda event: event[0])
    return [event[1:] for event in events]


def body(prompt, expert_ids, route_weights, gate_master, up_master, down_master, ffn_gain):
    group_count, shard_count, tp_count = (lax.axis_size(name) for name in ("gr", "fs", "tp"))
    g, f, t = (lax.axis_index(name) for name in ("gr", "fs", "tp"))
    where = jnp.stack([g, f, t]).astype(jnp.int32)
    local_in, rows, cols = gate_master.shape
    units = local_in * group_count // tp_count
    width = cols * tp_count // shard_count
    depth = prompt.shape[1]
    gain = ffn_gain.reshape(rows, 1)
    cut = [(which, unit) for unit in range(units) for which in (0, 1)][: units * CUT_EIGHTHS // 4]
    parts_of = {
        (which, unit): group_count if (which, unit) in cut else 1
        for unit in range(units)
        for which in (0, 1)
    }
    masters = (gate_master, up_master)
    serving = jax.ShapeDtypeStruct((units, rows * shard_count, width), BF16)
    down_serving = jax.ShapeDtypeStruct((units, *down_master.shape[1:2], depth), BF16)
    outer = shard_count // 2
    pairs = [(i, i ^ 1) for i in range(shard_count)]

    token_count = prompt.shape[0]
    xfloat = prompt.astype(F32)
    normed = (
        xfloat * lax.rsqrt(jnp.mean(xfloat * xfloat, axis=1, keepdims=True) + NORM_EPS)
    ).astype(BF16)
    local_experts = t * units + jnp.arange(units, dtype=jnp.int32)
    named = expert_ids[:, :, None] == local_experts[None, None, :]
    chosen = jnp.any(named, axis=1)
    earlier = jnp.tril(jnp.ones((token_count, token_count), BF16), -1)
    rank = jnp.dot(earlier, chosen.astype(BF16), preferred_element_type=F32).astype(jnp.int32)
    slot_ids = jnp.arange(SLOTS, dtype=jnp.int32)
    table = chosen.T[:, None, :] & (rank.T[:, None, :] == slot_ids[None, :, None])
    pair_weight = jnp.sum(jnp.where(named, route_weights[:, :, None], 0.0), axis=1)
    slot_weight = jnp.sum(jnp.where(table, pair_weight.T[:, None, :], 0.0), axis=2)[:, :, None]
    onehot = table.astype(BF16)
    token_onehot = onehot.transpose(0, 2, 1)
    routed = jnp.dot(
        onehot.reshape(units * SLOTS, token_count), normed, preferred_element_type=F32
    ).astype(BF16)

    last, count = routed, 0

    def step(kernel, *args):
        nonlocal last, count
        count += 1
        out = kernel(*args, last)
        last = out[-1] if isinstance(out, (list, tuple)) else out
        return out

    def swap(value):
        return lax.ppermute(value, "fs", pairs)

    by_gr, by_tp, arrived, pieces, folded = {}, {}, {}, {}, {}
    projections, down, mixed = None, None, None
    last = expert_ids
    for kind, key in plan(units, cut):
        if kind == "pack":
            which, unit = key
            parts = parts_of[key]
            packed = step(pack, masters[which], gain, where, unit, units, width, parts)
            by_gr[key] = [packed[0]] + [
                rotate(packed[shift % parts], "gr", shift) for shift in range(1, group_count)
            ]
        elif kind == "cast":
            own = step(cast, down_master, key, units)
            by_gr[key] = [own] + [rotate(own, "gr", shift) for shift in range(1, group_count)]
        elif kind == "tokens":
            last, routed = lax.optimization_barrier((last, routed))
            near_parts = [routed] + [rotate(routed, "fs", 2 * shift) for shift in range(1, outer)]
            last = routed
        elif kind == "near":
            near = step(stack, near_parts)
            far = swap(near)
        elif kind == "choose":
            by_tp[key] = []
            for shift in range(1, tp_count):
                by_tp[key].append(rotate(step(choose, by_gr[key], where, shift), "tp", shift))
        elif kind == "split":
            blocks = step(split, by_gr[key], by_tp[key], where, shard_count)
            arrived[key] = [blocks[0]] + [
                rotate(blocks[shift], "fs", shift) for shift in range(1, shard_count)
            ]
            if key not in cut:
                pieces[key] = arrived[key]
        elif kind == "stack":
            own = step(stack, arrived[key])
            pieces[key] = [own] + [rotate(own, "gr", shift) for shift in range(1, group_count)]
        elif kind == "project":
            parts = (parts_of[0, key], parts_of[1, key])
            *projections, hidden = step(
                up_project, where, near, far, pieces[0, key], pieces[1, key], projections, key, parts, serving
            )
            down, keep, out = step(
                down_project, where, hidden, by_gr[key], by_tp[key], down, key, down_serving
            )
            other = swap(out)
            sums = step(fold, keep, other, outer)
            folded[key] = (
                sums[0],
                [rotate(sums[shift], "fs", -2 * shift) for shift in range(1, outer)],
            )
        else:
            mixed = step(combine, slot_weight[key], token_onehot[key], *folded[key], mixed)

    mixed = mixed.reshape(tp_count, token_count // tp_count, depth)
    result = lax.dynamic_index_in_dim(mixed, t, 0, keepdims=False)
    for step in range(1, tp_count):
        target = lax.rem(t + step, tp_count)
        result = result + rotate(
            lax.dynamic_index_in_dim(mixed, target, 0, keepdims=False), "tp", step
        )
    return (*projections, down, result.astype(BF16))


def solution(mesh):
    in_specs = (
        P(("gr", "fs"), None),
        P(("gr", "fs"), None),
        P(("gr", "fs"), None),
        P("gr", "fs", "tp"),
        P("gr", "fs", "tp"),
        P("gr", "fs", "tp"),
        P("fs"),
    )
    out_specs = (
        P("tp", None, "fs"),
        P("tp", None, "fs"),
        P("tp", "fs", None),
        P(("gr", "fs", "tp"), None),
    )

    return jax.shard_map(body, mesh=mesh, in_specs=in_specs, out_specs=out_specs, check_vma=False)
```

```python
import functools
import heapq
import itertools

import jax
import jax.numpy as jnp
from jax import lax
from jax.experimental import pallas as pl
from jax.experimental.pallas import tpu as pltpu
from jax.sharding import PartitionSpec as P


NORM_EPS = 1e-06
SLOTS = 32
CUT_EIGHTHS = 2
TURNED_EIGHTHS = 3
LEAD = 1.0
CASTS = (3.0, 7.0, 8.7, 9.0)
WAITS = {"side": 0.5, "put": 0.7}
CUT, TURNED, WHOLE = 0, 1, 2


ANY = pl.BlockSpec(memory_space=pl.ANY)
SMEM = pl.BlockSpec(memory_space=pltpu.SMEM)
VMEM = pl.BlockSpec(memory_space=pltpu.VMEM)
BF16 = jnp.bfloat16
F32 = jnp.float32


def rotate(value, axis, step):
    count = lax.axis_size(axis)
    return lax.ppermute(value, axis, [(i, (i + step) % count) for i in range(count)])


def pack_kernel(parts, where_ref, after_ref, *refs):
    masters, gains, outs = refs[:parts], refs[parts : 2 * parts], refs[2 * parts :]
    for master, gain, out in zip(masters, gains, outs):
        out[0, 0] = (master[0] * gain[...]).astype(BF16)


def pack(master, gain, where, unit, units, width, parts, axis, after):
    _, rows, cols = master.shape
    held, blocks, part_rows = master.shape[0] // units, cols // width, rows // parts

    def row_part(p):
        return lambda k, c, w: (k * units + unit, (w[axis] + p) % parts, c)

    def gain_part(p):
        return lambda k, c, w: ((w[axis] + p) % parts, 0)

    out_spec = pl.BlockSpec((1, 1, part_rows, width), lambda k, c, w: (k, c, 0, 0))
    return pl.pallas_call(
        functools.partial(pack_kernel, parts),
        grid_spec=pltpu.PrefetchScalarGridSpec(
            num_scalar_prefetch=1,
            grid=(held, blocks),
            in_specs=[ANY]
            + [pl.BlockSpec((1, part_rows, width), row_part(p)) for p in range(parts)]
            + [pl.BlockSpec((part_rows, 1), gain_part(p)) for p in range(parts)],
            out_specs=[out_spec] * parts,
        ),
        out_shape=[jax.ShapeDtypeStruct((held, blocks, part_rows, width), BF16)] * parts,
        name="pack",
    )(where, after, *([master] * parts), *([gain] * parts))


def choose_kernel(group_count, tp_count, held, tp_step, where_ref, after_ref, *refs):
    by_gr, (out, stage, sem) = refs[:group_count], refs[group_count:]
    target = lax.rem(where_ref[2] + tp_step, tp_count)
    gr_step = lax.rem(where_ref[0] + group_count - lax.div(target, held), group_count)
    for s in range(group_count):

        @pl.when(gr_step == s)
        def _(s=s):
            copy = pltpu.make_async_copy(by_gr[s].at[lax.rem(target, held)], stage, sem)
            copy.start()
            copy.wait()

    copy = pltpu.make_async_copy(stage, out, sem)
    copy.start()
    copy.wait()


def choose(by_gr, where, tp_step, after):
    held, *shape = by_gr[0].shape
    return pl.pallas_call(
        functools.partial(choose_kernel, len(by_gr), lax.axis_size("tp"), held, tp_step),
        in_specs=[SMEM] + [ANY] * (len(by_gr) + 1),
        out_specs=ANY,
        out_shape=jax.ShapeDtypeStruct(tuple(shape), BF16),
        scratch_shapes=[pltpu.VMEM(tuple(shape), BF16), pltpu.SemaphoreType.DMA],
        name="choose",
    )(where, after, *by_gr)


def stack_kernel(count, after_ref, *refs):
    ins, (out, stage, in_sem, out_sem) = refs[:count], refs[count:]

    def fetch(i):
        return pltpu.make_async_copy(ins[i], stage.at[i], in_sem.at[i])

    def flush(i):
        return pltpu.make_async_copy(stage.at[i], out.at[i], out_sem.at[i])

    for i in range(count):
        fetch(i).start()
    for i in range(count):
        fetch(i).wait()
        flush(i).start()
    for i in range(count):
        flush(i).wait()


def stack(values, after):
    count, shape = len(values), (len(values), *values[0].shape)
    return pl.pallas_call(
        functools.partial(stack_kernel, count),
        in_specs=[ANY] * (count + 1),
        out_specs=ANY,
        out_shape=jax.ShapeDtypeStruct(shape, BF16),
        scratch_shapes=[
            pltpu.VMEM(shape, BF16),
            pltpu.SemaphoreType.DMA((count,)),
            pltpu.SemaphoreType.DMA((count,)),
        ],
        name="stack",
    )(after, *values)


def split_kernel(group_count, tp_count, shard_count, held, where_ref, after_ref, *refs):
    by_gr, by_tp = refs[:group_count], refs[group_count : group_count + tp_count - 1]
    outs = refs[group_count + tp_count - 1 : group_count + tp_count - 1 + shard_count]
    stage, in_sem, out_sem = refs[-3:]
    g, f, t = where_ref[0], where_ref[1], where_ref[2]
    blocks = by_gr[0].shape[1]

    def source(step):
        target = lax.rem(f + step, shard_count)
        return lax.div(target, blocks), lax.rem(target, blocks)

    for step in range(shard_count):
        column, block = source(step)
        own_gr = lax.rem(g + group_count - lax.div(t, held), group_count)
        tp_step = lax.rem(t + tp_count - column, tp_count)
        for s in range(group_count):

            @pl.when((tp_step == 0) & (own_gr == s))
            def _(s=s):
                pltpu.make_async_copy(
                    by_gr[s].at[lax.rem(t, held), block], stage.at[step], in_sem.at[step]
                ).start()

        for s in range(1, tp_count):

            @pl.when(tp_step == s)
            def _(s=s):
                pltpu.make_async_copy(by_tp[s - 1].at[block], stage.at[step], in_sem.at[step]).start()

    for step in range(shard_count):
        pltpu.make_async_copy(stage.at[step], stage.at[step], in_sem.at[step]).wait()
        pltpu.make_async_copy(stage.at[step], outs[step], out_sem.at[step]).start()
    for step in range(shard_count):
        pltpu.make_async_copy(stage.at[step], outs[step], out_sem.at[step]).wait()


def split(by_gr, by_tp, where, shard_count, after):
    held, _, rows, width = by_gr[0].shape
    piece = jax.ShapeDtypeStruct((rows, width), BF16)
    return pl.pallas_call(
        functools.partial(split_kernel, len(by_gr), len(by_tp) + 1, shard_count, held),
        in_specs=[SMEM] + [ANY] * (len(by_gr) + len(by_tp) + 1),
        out_specs=[ANY] * shard_count,
        out_shape=[piece] * shard_count,
        scratch_shapes=[
            pltpu.VMEM((shard_count, rows, width), BF16),
            pltpu.SemaphoreType.DMA((shard_count,)),
            pltpu.SemaphoreType.DMA((shard_count,)),
        ],
        name="split",
    )(where, after, *by_gr, *by_tp)


def side_kernel(count, route, group_count, parts, unit, fresh, which, where_ref, after_ref, near, far, *refs):
    ins, rest = refs[:count], refs[count:]
    other_ref, rest = (None, rest) if which is None else (rest[0], rest[1:])
    if not fresh:
        rest = rest[1:]
    out, result_ref, tokens, buf, token_sem, in_sem, out_sem = rest
    g, f, t = where_ref[0], where_ref[1], where_ref[2]
    outer, slots, depth = near.shape[0], tokens.shape[1], tokens.shape[2]
    shard_count = 2 * outer
    whole = buf.shape[0] // shard_count
    rows = whole // parts

    def place(index):
        part, step = divmod(index, shard_count)
        source = lax.rem(f + shard_count - step, shard_count)
        own = t if route == TURNED else g
        start = source * whole + lax.rem(own + parts - part, parts) * rows
        return pl.ds(pl.multiple_of(start, rows), rows)

    def fetch(index, entry=None):
        part, step = divmod(index, shard_count)
        if route == WHOLE:
            src = ins[index]
        else:
            skip = group_count - 1 if route == TURNED and part else 0
            src = ins[part + skip if entry is None else entry].at[step]
        return pltpu.make_async_copy(src, buf.at[place(index)], in_sem.at[index])

    def flush(index):
        at = place(index)
        return pltpu.make_async_copy(buf.at[at], out.at[unit, at, :], out_sem.at[index])

    token_copies = [
        pltpu.make_async_copy(
            src.at[:, pl.ds(unit * slots, slots), :],
            tokens.at[pl.ds(i * outer, outer)],
            token_sem.at[i],
        )
        for i, src in enumerate((near, far))
    ]
    for copy in token_copies:
        copy.start()
    for index in range(shard_count * parts):
        if route == TURNED and index < shard_count:
            gr_step = lax.rem(g + group_count - t, group_count)
            for entry in range(group_count):
                pl.when(gr_step == entry)(fetch(index, entry).start)
        else:
            fetch(index).start()
    for copy in token_copies:
        copy.wait()
    for index in range(shard_count * parts):
        fetch(index).wait()
        flush(index).start()
    rows_in = tokens[...].reshape(shard_count * slots, depth)
    product = jnp.dot(rows_in, buf[...], preferred_element_type=F32)
    if which is None:
        result_ref[...] = product
    else:
        gate, up = (product, other_ref[...]) if which == 0 else (other_ref[...], product)
        result_ref[...] = (gate / (1.0 + jnp.exp(-gate)) * up).astype(BF16)
    for index in range(shard_count * parts):
        flush(index).wait()


def project_side(where, near, far, pieces, out, other, unit, which, route, out_shape, after):
    width = out_shape.shape[2]
    shard_count, depth = 2 * near.shape[0], near.shape[2]
    slots = near.shape[1] // out_shape.shape[0]
    token_count = shard_count * slots
    fresh, second = out is None, other is not None
    group_count = lax.axis_size("gr")
    parts = {CUT: group_count, TURNED: lax.axis_size("tp"), WHOLE: 1}[route]
    operands = [where, after, near, far, *pieces] + ([other] if second else []) + ([] if fresh else [out])
    specs = [SMEM] + [ANY] * (3 + len(pieces)) + ([VMEM] if second else []) + ([] if fresh else [ANY])
    return pl.pallas_call(
        functools.partial(
            side_kernel, len(pieces), route, group_count, parts, unit, fresh, which if second else None
        ),
        in_specs=specs,
        out_specs=[ANY, VMEM],
        out_shape=[out_shape, jax.ShapeDtypeStruct((token_count, width), BF16 if second else F32)],
        scratch_shapes=[
            pltpu.VMEM((shard_count, slots, depth), BF16),
            pltpu.VMEM((depth, width), BF16),
            pltpu.SemaphoreType.DMA((2,)),
            pltpu.SemaphoreType.DMA((shard_count * parts,)),
            pltpu.SemaphoreType.DMA((shard_count * parts,)),
        ],
        input_output_aliases={} if fresh else {len(operands) - 1: 0},
        name="project_side",
    )(*operands)


def down_fetch(by_gr, by_tp, held, where_ref, buf, in_sem):
    group_count = len(by_gr)
    g, t = where_ref[0], where_ref[2]
    own_gr = lax.rem(g + group_count - lax.div(t, held), group_count)
    for s in range(group_count):

        @pl.when(own_gr == s)
        def _(s=s):
            pltpu.make_async_copy(by_gr[s].at[lax.rem(t, held)], buf.at[0], in_sem.at[0]).start()

    for s, value in enumerate(by_tp):
        pltpu.make_async_copy(value, buf.at[s + 1], in_sem.at[s + 1]).start()


def down_columns(where_ref, step, tp_count, cols):
    column = lax.rem(where_ref[2] + tp_count - step, tp_count) * cols
    return pl.ds(pl.multiple_of(column, cols), cols)


def put_down_kernel(group_count, tp_count, held, unit, where_ref, after_ref, *refs):
    by_gr, by_tp = refs[:group_count], refs[group_count : group_count + tp_count - 1]
    out, done_ref, buf, in_sem, out_sem = refs[-5:]
    down_fetch(by_gr, by_tp, held, where_ref, buf, in_sem)

    def flush(s):
        columns = down_columns(where_ref, s, tp_count, buf.shape[2])
        return pltpu.make_async_copy(buf.at[s], out.at[unit, :, columns], out_sem.at[s])

    for s in range(tp_count):
        pltpu.make_async_copy(buf.at[s], buf.at[s], in_sem.at[s]).wait()
        flush(s).start()
    done_ref[...] = jnp.zeros_like(done_ref)
    for s in range(tp_count):
        flush(s).wait()


def put_down(where, by_gr, by_tp, out, unit, out_shape, after):
    held, rows, cols = by_gr[0].shape
    tp_count = len(by_tp) + 1
    fresh = out is None
    operands = [where, after, *by_gr, *by_tp] + ([] if fresh else [out])
    return pl.pallas_call(
        functools.partial(put_down_kernel, len(by_gr), tp_count, held, unit),
        in_specs=[SMEM] + [ANY] * (len(operands) - 1),
        out_specs=[ANY, VMEM],
        out_shape=[out_shape, jax.ShapeDtypeStruct((8, 128), F32)],
        scratch_shapes=[
            pltpu.VMEM((tp_count, rows, cols), BF16),
            pltpu.SemaphoreType.DMA((tp_count,)),
            pltpu.SemaphoreType.DMA((tp_count,)),
        ],
        input_output_aliases={} if fresh else {len(operands) - 1: 0},
        name="put_down",
    )(*operands)


def down_kernel(group_count, tp_count, held, where_ref, after_ref, hidden_ref, *refs):
    by_gr, by_tp = refs[:group_count], refs[group_count : group_count + tp_count - 1]
    near_ref, far_ref, buf, part, in_sem = refs[-5:]
    down_fetch(by_gr, by_tp, held, where_ref, buf, in_sem)
    for s in range(tp_count):
        pltpu.make_async_copy(buf.at[s], buf.at[s], in_sem.at[s]).wait()
        part[:, down_columns(where_ref, s, tp_count, buf.shape[2])] = jnp.dot(
            hidden_ref[...], buf[s], preferred_element_type=F32
        ).astype(BF16)
    half = near_ref.shape[0]
    near_ref[...] = part[:half]
    far_ref[...] = part[half:]


def down_project(where, hidden, by_gr, by_tp, after):
    held, rows, cols = by_gr[0].shape
    token_count, _ = hidden.shape
    tp_count = len(by_tp) + 1
    depth = cols * tp_count
    half = jax.ShapeDtypeStruct((token_count // 2, depth), BF16)
    operands = [where, after, hidden, *by_gr, *by_tp]
    return pl.pallas_call(
        functools.partial(down_kernel, len(by_gr), tp_count, held),
        in_specs=[SMEM, ANY, VMEM] + [ANY] * (len(operands) - 3),
        out_specs=[VMEM, VMEM],
        out_shape=[half, half],
        scratch_shapes=[
            pltpu.VMEM((tp_count, rows, cols), BF16),
            pltpu.VMEM((token_count, depth), BF16),
            pltpu.SemaphoreType.DMA((tp_count,)),
        ],
        name="down_project",
    )(*operands)


def fold_kernel(outer, after_ref, keep_ref, other_ref, own_ref, *sends):
    total = keep_ref[...].astype(F32) + other_ref[...].astype(F32)
    slots = own_ref.shape[0]
    own_ref[...] = total[:slots]
    for step in range(1, outer):
        sends[step - 1][...] = total[step * slots : (step + 1) * slots].astype(BF16)


def fold(keep, other, outer, after):
    slots, depth = keep.shape[0] // outer, keep.shape[1]
    return pl.pallas_call(
        functools.partial(fold_kernel, outer),
        in_specs=[ANY, VMEM, VMEM],
        out_specs=[VMEM] * outer,
        out_shape=[jax.ShapeDtypeStruct((slots, depth), F32)]
        + [jax.ShapeDtypeStruct((slots, depth), BF16)] * (outer - 1),
        name="fold",
    )(after, keep, other)


def combine_kernel(count, parts, first, after_ref, weight_ref, own_ref, *refs):
    others, onehots = refs[:count], refs[count : count + parts]
    sums, outs = refs[count + parts : -parts], refs[-parts:]
    total = own_ref[...]
    for other in others:
        total = total + other[...].astype(F32)
    term = (total * weight_ref[...]).astype(BF16)
    for i in range(parts):
        share = lax.dot_general(
            onehots[i][...], term, (((1,), (0,)), ((), ())), preferred_element_type=F32
        )
        outs[i][...] = (share if first else sums[i][...] + share).astype(outs[i].dtype)


def combine(weight, onehots, own, others, sums, dtype, after):
    first = sums is None
    parts = len(onehots)
    shape = jax.ShapeDtypeStruct((onehots[0].shape[0], own.shape[1]), dtype)
    operands = [after, weight, own, *others, *onehots, *([] if first else sums)]
    return pl.pallas_call(
        functools.partial(combine_kernel, len(others), parts, first),
        in_specs=[ANY] + [VMEM] * (len(operands) - 1),
        out_specs=[VMEM] * parts,
        out_shape=[shape] * parts,
        name="combine",
    )(*operands)


def cast_kernel(after_ref, in_ref, out_ref):
    out_ref[...] = in_ref[...].astype(BF16)


def cast(master, unit, units, after):
    local_in, rows, cols = master.shape
    held, half = local_in // units, rows // 2
    return pl.pallas_call(
        cast_kernel,
        grid=(held, 2),
        in_specs=[ANY, pl.BlockSpec((1, half, cols), lambda k, i: (k * units + unit, i, 0))],
        out_specs=pl.BlockSpec((1, half, cols), lambda k, i: (k, i, 0)),
        out_shape=jax.ShapeDtypeStruct((held, rows, cols), BF16),
        name="cast",
    )(after, master)


def choose_routes(units, held):
    both = (0, 1)
    keys = [(which, unit) for unit in range(units) for which in both]
    cut, turned = (len(keys) * n // 8 for n in (CUT_EIGHTHS, TURNED_EIGHTHS if held == 1 else 0))
    return {
        key: CUT if i < cut else TURNED if i < cut + turned else WHOLE for i, key in enumerate(keys)
    }


def plan(units, routes):
    keys = sorted(routes, key=lambda key: (routes[key] == WHOLE, key[1], key[0]))
    parts = [key for key in keys if routes[key] != WHOLE]
    cuts = [key for key in parts if routes[key] == CUT]
    turns = [key for key in parts if routes[key] == TURNED]
    order = []
    for i in range(max(len(cuts), len(turns))):
        order += cuts[i : i + 1] + turns[i : i + 1]
    rank = {
        unit: (CUT in (routes[0, unit], routes[1, unit]), routes[0, unit] != routes[1, unit], unit)
        for unit in range(units)
    }
    whole = sorted((key for key in keys if routes[key] == WHOLE), key=lambda key: rank[key[1]])
    downs = sorted(range(units), key=rank.get)
    events, tie = [], itertools.count()

    def at(time, kind, key):
        heapq.heappush(events, (time, next(tie), kind, key))

    for i, key in enumerate(order):
        at(0.22 * i, "pack", key)
    at(0.43 if order else 0.0, "tokens", None)
    for i, key in enumerate(whole):
        at(0.22 * len(order) + 0.3 * i, "pack", key)
    for i, unit in enumerate(downs):
        at(CASTS[min(i, len(CASTS) - 1)] + 0.1 * i, "cast", unit)
    free = {"gr": 0.1, "fs": 0.1, "tp": 0.1}
    missing = {unit: 3 for unit in range(units)}
    now, steps = 0.0, []

    def move(axis, amount, kind, key):
        free[axis] = max(free[axis], now) + amount
        at(free[axis] + WAITS.get(kind, 0.0) * (key not in cuts), kind, key)

    costs = {"pack": 0.25, "cast": 0.2, "choose": 0.2, "split": 0.5, "stack": 0.15, "side": 0.25, "put": 0.2}
    while events:
        time, _, kind, key = heapq.heappop(events)
        late = free["fs"] - LEAD - max(now, time)
        if kind == "split" and late > 0.01:
            at(free["fs"] - LEAD, kind, key)
            continue
        steps.append((kind, key))
        now = max(now, time) + costs.get(kind, 0.3)
        route = routes.get(key, WHOLE)
        size = 2 if route == WHOLE else 1
        if kind == "tokens":
            move("fs", 2, "near", None)
        elif kind == "pack" and route == TURNED:
            move("tp", 1, "split", key)
        elif kind in ("pack", "cast"):
            move("gr", size, "choose", key)
        elif kind == "choose":
            down = key in missing
            move("tp", size, "put" if down else "split", key)
        elif kind == "split":
            move("fs", 2 * size, "side" if route == WHOLE else "stack", key)
        elif kind == "stack":
            move("gr", 2, "side" if route == CUT else "turn", key)
        elif kind == "turn":
            move("tp", 2, "side", key)
        elif kind in ("side", "put"):
            unit = key[1] if kind == "side" else key
            missing[unit] -= 1
            if not missing[unit]:
                at(now, "project", unit)
        elif kind == "project":
            now += 0.3
            move("fs", 0.5, "settle", key)
    final = [key for kind, key in steps if kind == "project"][-1]
    steps.remove(("put", final))
    steps.insert(steps.index(("project", final)) + 1, ("put", final))
    return steps


def body(prompt, expert_ids, route_weights, gate_master, up_master, down_master, ffn_gain):
    group_count, shard_count, tp_count = (lax.axis_size(name) for name in ("gr", "fs", "tp"))
    g, f, t = (lax.axis_index(name) for name in ("gr", "fs", "tp"))
    where = jnp.stack([g, f, t]).astype(jnp.int32)
    local_in, rows, cols = gate_master.shape
    units = local_in * group_count // tp_count
    width = cols * tp_count // shard_count
    depth = prompt.shape[1]
    gain = ffn_gain.reshape(rows, 1)
    routes = choose_routes(units, local_in // units)
    masters = (gate_master, up_master)
    serving = jax.ShapeDtypeStruct((units, rows * shard_count, width), BF16)
    down_serving = jax.ShapeDtypeStruct((units, *down_master.shape[1:2], depth), BF16)
    outer = shard_count // 2
    pairs = [(i, i ^ 1) for i in range(shard_count)]

    token_count = prompt.shape[0]
    xfloat = prompt.astype(F32)
    normed = (
        xfloat * lax.rsqrt(jnp.mean(xfloat * xfloat, axis=1, keepdims=True) + NORM_EPS)
    ).astype(BF16)
    local_experts = t * units + jnp.arange(units, dtype=jnp.int32)
    named = expert_ids[:, :, None] == local_experts[None, None, :]
    chosen = jnp.any(named, axis=1)
    earlier = jnp.tril(jnp.ones((token_count, token_count), BF16), -1)
    rank = jnp.dot(earlier, chosen.astype(BF16), preferred_element_type=F32).astype(jnp.int32)
    slot_ids = jnp.arange(SLOTS, dtype=jnp.int32)
    table = chosen.T[:, None, :] & (rank.T[:, None, :] == slot_ids[None, :, None])
    pair_weight = jnp.sum(jnp.where(named, route_weights[:, :, None], 0.0), axis=1)
    slot_weight = jnp.sum(jnp.where(table, pair_weight.T[:, None, :], 0.0), axis=2)[:, :, None]
    onehot = table.astype(BF16)
    token_onehot = onehot.transpose(0, 2, 1).reshape(units, tp_count, token_count // tp_count, SLOTS)
    token_onehot = [
        lax.dynamic_index_in_dim(token_onehot, lax.rem(t + shift, tp_count), 1, keepdims=False)
        for shift in range(tp_count)
    ]
    routed = jnp.dot(
        onehot.reshape(units * SLOTS, token_count), normed, preferred_element_type=F32
    ).astype(BF16)

    last, count = routed, 0

    def step(kernel, *args):
        nonlocal last, count
        count += 1
        out = kernel(*args, last)
        last = out[-1] if isinstance(out, (list, tuple)) else out
        return out

    def swap(value):
        return lax.ppermute(value, "fs", pairs)

    by_gr, by_tp, arrived, pieces, folded = {}, {}, {}, {}, {}
    projections, products = [None, None], {}
    down, mixed, result, settled = None, None, None, 0
    last = expert_ids
    for kind, key in plan(units, routes):
        if kind == "pack":
            which, unit = key
            master = masters[which]
            if routes[key] == TURNED:
                packed = step(pack, master, gain, where, unit, units, width, tp_count, 2)
                by_gr[key] = packed[:1]
                by_tp[key] = [
                    rotate(packed[shift], "tp", shift).reshape(packed[0].shape[1:])
                    for shift in range(1, tp_count)
                ]
            else:
                parts = group_count if routes[key] == CUT else 1
                packed = step(pack, master, gain, where, unit, units, width, parts, 0)
                by_gr[key] = [packed[0]] + [
                    rotate(packed[shift % parts], "gr", shift) for shift in range(1, group_count)
                ]
        elif kind == "cast":
            own = step(cast, down_master, key, units)
            by_gr[key] = [own] + [rotate(own, "gr", shift) for shift in range(1, group_count)]
        elif kind == "tokens":
            last, routed = lax.optimization_barrier((last, routed))
            near_parts = [routed] + [rotate(routed, "fs", 2 * shift) for shift in range(1, outer)]
            last = routed
        elif kind == "near":
            near = step(stack, near_parts)
            far = swap(near)
        elif kind == "choose":
            by_tp[key] = []
            for shift in range(1, tp_count):
                by_tp[key].append(rotate(step(choose, by_gr[key], where, shift), "tp", shift))
        elif kind == "split":
            blocks = step(split, by_gr[key], by_tp[key], where, shard_count)
            arrived[key] = [blocks[0]] + [
                rotate(blocks[shift], "fs", shift) for shift in range(1, shard_count)
            ]
            if routes[key] == WHOLE:
                pieces[key] = arrived[key]
        elif kind == "stack":
            own = step(stack, arrived[key])
            pieces[key] = [own] + [rotate(own, "gr", shift) for shift in range(1, group_count)]
        elif kind == "turn":
            by_step = [value[None] for value in pieces[key]]
            for shift in range(1, tp_count):
                pieces[key] = pieces[key] + [rotate(step(choose, by_step, where, shift), "tp", shift)]
        elif kind == "side":
            which, unit = key
            projections[which], products[unit] = step(
                project_side, where, near, far, pieces[key], projections[which], products.get(unit),
                unit, which, routes[key], serving,
            )
        elif kind == "put":
            down, _ = step(put_down, where, by_gr[key], by_tp[key], down, key, down_serving)
        elif kind == "project":
            keep, out = step(down_project, where, products[key], by_gr[key], by_tp[key])
            other = swap(out)
            sums = step(fold, keep, other, outer)
            folded[key] = (
                sums[0],
                [rotate(sums[shift], "fs", -2 * shift) for shift in range(1, outer)],
            )
        else:
            settled += 1
            final = settled == units
            onehots = [value[key] for value in token_onehot]
            shares = step(
                combine, slot_weight[key], onehots, *folded[key], None if final else mixed, BF16 if final else F32
            )
            mixed = None if final else shares
            if settled >= units - 1:
                result = shares[0].astype(F32) if result is None else result + shares[0]
                for shift in range(1, tp_count):
                    result = result + rotate(shares[shift], "tp", shift)
    return (*projections, down, result.astype(BF16))


def solution(mesh):
    in_specs = (
        P(("gr", "fs"), None),
        P(("gr", "fs"), None),
        P(("gr", "fs"), None),
        P("gr", "fs", "tp"),
        P("gr", "fs", "tp"),
        P("gr", "fs", "tp"),
        P("fs"),
    )
    out_specs = (
        P("tp", None, "fs"),
        P("tp", None, "fs"),
        P("tp", "fs", None),
        P(("gr", "fs", "tp"), None),
    )

    return jax.shard_map(body, mesh=mesh, in_specs=in_specs, out_specs=out_specs, check_vma=False)
```
